32 devices in a mesh: sp: 4 (over z), dp: 8 (over y, x, core).
Axes of the slice: x: 2, y: 2, z: 4, core: 2. Of those that a mesh axis runs over, the one named last changes fastest.
Arguments:
- queries: bfloat16 [8, 512, 1024], P('dp', 'sp'), may hold values from -6 to 6
- key_rows: bfloat16 [8, 512, 1024], P('dp', 'sp'), may hold values from -6 to 6
- value_rows: bfloat16 [8, 512, 1024], P('dp', 'sp'), may hold values from -6 to 6
- break_offset: bfloat16 [8, 512, 16], P('dp', 'sp'), may hold values from 1.5 to 15
- hidden_in: bfloat16 [8, 512, 2048], P('dp', 'sp'), may hold values from -6 to 6
- gate_weight: bfloat16 [2048, 1024], P('dp', 'sp'), may hold values from -0.125 to 0.125
- out_weight: bfloat16 [1024, 2048], P('sp', 'dp'), may hold values from -0.1875 to 0.1875
Outputs:
- mixed: bfloat16 [8, 512, 2048], P('dp', 'sp')
The draws below stay inside these ranges and needn't reach their ends.
All inputs are finite; a program needn't handle non-finite values.
Results may differ from the reference program's by a relative error of at most 0.0063.
Values may be sent and summed in bfloat16 or wider, within the bound.
A program may use at most 64 MiB of HBM per device.

```python
import math
import jax
import jax.numpy as jnp
from jax import lax

D = 2048
HEADS = 16
HD = 64
HH = 1024
BATCH = 8
LENGTH = 512


def draw_break_offset(key, part):
    head_key, base_key, span_key, rough_key = jax.random.split(jax.random.fold_in(key, 17), 4)
    fast_share = 0.5
    fast_heads = jax.random.uniform(head_key, (HEADS,)) < fast_share
    spread = jax.random.uniform(base_key, (HEADS,))
    base = jnp.where(fast_heads, 3.0 + spread, math.log(LENGTH) + 1.0 + spread)
    spans = jax.random.uniform(span_key, (BATCH, LENGTH // 64, HEADS), minval=-0.7, maxval=0.7)
    spans = jnp.repeat(spans, 64, axis=1)
    rough = jax.random.uniform(rough_key, (BATCH, LENGTH, HEADS), minval=-0.5, maxval=0.5)
    return (base[None, None, :] + spans + rough).astype(jnp.bfloat16)


def block_levels(stream_key, shape, cuts, smallest, high):
    gain, own = 1.0, jax.random.fold_in(stream_key, 6)
    for dim, parts in cuts:
        heights = jnp.exp(jax.random.uniform(jax.random.fold_in(own, dim), (parts,), jnp.float32, smallest / len(cuts), high / len(cuts)))
        gain = gain * jnp.repeat(heights, shape[dim] // parts).reshape([-1 if axis == dim else 1 for axis in range(len(shape))])
    return gain


def bell_draw(rng, dims, scale, bound, cuts=(), kind=jnp.bfloat16):
    entries = jax.random.normal(rng, dims, jnp.float32) * scale
    if len(cuts) > 0:
        entries = block_levels(rng, dims, cuts, -0.22, 0.18) * entries
    return jnp.clip(entries, min=-bound, max=bound).astype(kind)


def setup_inputs(seed: int = 0) -> dict:
    streams_of = jax.random.split(jax.random.key(seed), 8)
    return {
        "queries": bell_draw(streams_of[0], (BATCH, LENGTH, HH), 1.0, 6.0, ((0, 8), (1, 4))),
        "key_rows": bell_draw(streams_of[1], (BATCH, LENGTH, HH), 1.0, 6.0, ((0, 8), (1, 4))),
        "value_rows": bell_draw(streams_of[2], (BATCH, LENGTH, HH), 1.0, 6.0, ((0, 8), (1, 4))),
        "break_offset": draw_break_offset(jax.random.fold_in(streams_of[7], 71), 0),
        "hidden_in": bell_draw(streams_of[4], (BATCH, LENGTH, D), 1.0, 6.0, ((0, 8), (1, 4))),
        "gate_weight": bell_draw(streams_of[5], (D, HH), D ** -0.5, 0.125, ((0, 8), (1, 4))),
        "out_weight": bell_draw(streams_of[6], (HH, D), HH ** -0.5, 0.1875, ((0, 4), (1, 8))),
    }


eps_norm = 1e-05

def stick_heads(queries, key_rows, value_rows, offsets):
    block_rows = min(512, LENGTH)
    score_scale = HD ** (-0.5)
    key_pos = jnp.arange(LENGTH).astype(jnp.int32)

    def one_block(block_index):
        first_row = (block_index * block_rows).astype(jnp.int32)
        query_block = lax.dynamic_slice_in_dim(queries, first_row, block_rows, 1)
        scores = jnp.einsum('hqd,hkd->hqk', query_block, key_rows) * score_scale - offsets[:, None, :]
        query_pos = first_row + jnp.arange(block_rows).astype(jnp.int32)
        earlier = key_pos[None, :] < query_pos[:, None]
        keep_log = jnp.where(earlier, jax.nn.log_sigmoid(-scores), 0.0)
        later_sum = lax.cumsum(keep_log, axis=2, reverse=True) - keep_log
        weights = jnp.where(earlier, jnp.exp(jax.nn.log_sigmoid(scores) + later_sum), 0.0).astype(jnp.bfloat16)
        return jnp.einsum('hqk,hkd->hqd', weights.astype(jnp.float32), value_rows)
    blocks = lax.map(one_block, jnp.arange(LENGTH // block_rows).astype(jnp.int32))
    return blocks.transpose(1, 0, 2, 3).reshape(HEADS, LENGTH, HD)

def reference(queries, key_rows, value_rows, break_offset, hidden_in, gate_weight, out_weight):

    def heads_first(array):
        return array.astype(jnp.float32).reshape(LENGTH, HEADS, HD).transpose(1, 0, 2)

    def one_sequence(inputs):
        seq_queries, seq_keys, seq_values, seq_offsets, seq_hidden = inputs
        heads_out = stick_heads(heads_first(seq_queries), heads_first(seq_keys), heads_first(seq_values), seq_offsets.astype(jnp.float32).T)
        mean_sq = lax.optimization_barrier(jnp.mean(heads_out * heads_out, axis=2, keepdims=True))
        normed = (heads_out * lax.rsqrt(mean_sq + eps_norm)).astype(jnp.bfloat16)
        normed = normed.transpose(1, 0, 2).reshape(LENGTH, HH)
        gate_act = jax.nn.silu(jnp.dot(seq_hidden, gate_weight, preferred_element_type=jnp.float32))
        gated = (normed.astype(jnp.float32) * gate_act).astype(jnp.bfloat16)
        return jnp.dot(gated, out_weight, preferred_element_type=jnp.float32).astype(jnp.bfloat16)
    return lax.map(one_sequence, (queries, key_rows, value_rows, break_offset, hidden_in))
```

```python
import functools
import math
import jax
import jax.numpy as jnp
from jax import lax
from jax.experimental import pallas as pl
from jax.experimental.pallas import tpu as pltpu
from jax.sharding import PartitionSpec as P

eps_norm = 1e-05
QKV_FIRST = True


def stick_blocks(head_queries, head_keys, head_values, head_offsets):
    groups, length, head_size = head_queries.shape
    block_rows = min(512, length)
    block_count = length // block_rows
    score_scale = head_size ** (-0.5)
    query_blocks = head_queries.reshape(groups, block_count, block_rows, head_size)

    def one_block(block_index):
        query_block = lax.dynamic_index_in_dim(query_blocks, block_index, 1, keepdims=False)
        query_pos = block_index * block_rows + jnp.arange(block_rows, dtype=jnp.int32)

        def key_step(step_turn, carry):
            running, carried = carry
            key_first = (block_index - step_turn) * block_rows
            key_block = lax.dynamic_slice_in_dim(head_keys, key_first, block_rows, 1)
            value_block = lax.dynamic_slice_in_dim(head_values, key_first, block_rows, 1)
            offset_block = lax.dynamic_slice_in_dim(head_offsets, key_first, block_rows, 1)
            scores = jnp.einsum(
                "gqd,gkd->gqk", query_block, key_block, preferred_element_type=jnp.float32
            )
            scores = scores * score_scale - offset_block[:, None, :]
            key_pos = key_first + jnp.arange(block_rows, dtype=jnp.int32)
            earlier = key_pos[None, :] < query_pos[:, None]
            keep_log = jnp.where(earlier, jax.nn.log_sigmoid(-scores), 0.0)
            later_sum = lax.cumsum(keep_log, axis=2, reverse=True) - keep_log + carried
            weights = jnp.where(
                earlier, jnp.exp(jax.nn.log_sigmoid(scores) + later_sum), 0.0
            ).astype(jnp.bfloat16)
            running = running + jnp.einsum(
                "gqk,gkd->gqd", weights, value_block, preferred_element_type=jnp.float32
            )
            carried = carried + jnp.sum(keep_log, axis=2, keepdims=True)
            return (running, carried)

        start_carry = (
            jnp.zeros((groups, block_rows, head_size), jnp.float32),
            jnp.zeros((groups, block_rows, 1), jnp.float32),
        )
        running, carried = lax.fori_loop(0, block_index + 1, key_step, start_carry)
        return running

    outputs = lax.map(one_block, jnp.arange(block_count, dtype=jnp.int32))
    return outputs.transpose(1, 0, 2, 3).reshape(groups, length, head_size)


def attend(pieces):
    head_queries, head_keys, head_values, head_offsets = pieces
    item_count, length, feature_count = head_queries.shape
    heads_dev = head_offsets.shape[2]
    head_size = feature_count // heads_dev

    def split_heads(array):
        return (
            array.reshape(item_count, length, heads_dev, head_size)
            .transpose(0, 2, 1, 3)
            .reshape(item_count * heads_dev, length, head_size)
        )

    offsets = (
        head_offsets.transpose(0, 2, 1).reshape(item_count * heads_dev, length).astype(jnp.float32)
    )
    heads_out = stick_blocks(
        split_heads(head_queries), split_heads(head_keys), split_heads(head_values), offsets
    )
    mean_sq = jnp.mean(heads_out * heads_out, axis=2, keepdims=True)
    normed = (heads_out * lax.rsqrt(mean_sq + eps_norm)).astype(jnp.bfloat16)
    return (
        normed.reshape(item_count, heads_dev, length, head_size)
        .transpose(0, 2, 1, 3)
        .reshape(item_count, length, feature_count)
    )


def shards(queries, key_rows, value_rows, break_offset, hidden_in, gate_weight, out_weight):
    tokens = hidden_in[0]
    gate_rows, out_cols = (
        lax.all_gather(gate_weight, "sp", axis=1, tiled=True),
        lax.all_gather(out_weight, "sp", axis=0, tiled=True),
    )
    gate_pre = jnp.dot(
        tokens,
        lax.all_gather(gate_rows, "dp", axis=0, tiled=True),
        preferred_element_type=jnp.float32,
    )
    gate_act = jax.nn.silu(gate_pre)
    normed = attend(
        (
            lax.all_to_all(queries, "sp", split_axis=2, concat_axis=1, tiled=True),
            lax.all_to_all(key_rows, "sp", split_axis=2, concat_axis=1, tiled=True),
            lax.all_to_all(value_rows, "sp", split_axis=2, concat_axis=1, tiled=True),
            lax.all_to_all(break_offset, "sp", split_axis=2, concat_axis=1, tiled=True),
        )
    )
    returned = lax.all_to_all(normed, "sp", split_axis=1, concat_axis=2, tiled=True)
    gated_rows = (returned[0].astype(jnp.float32) * gate_act).astype(jnp.bfloat16)
    mixed_rows = jnp.dot(
        gated_rows,
        lax.all_gather(out_cols, "dp", axis=1, tiled=True),
        preferred_element_type=jnp.float32,
    )
    return mixed_rows.astype(jnp.bfloat16)[None]


log2_e = math.log2(math.e)
f32, bf16 = jnp.float32, jnp.bfloat16


def plane_kernel(
    n_sp,
    n_dp,
    head_size,
    q_ref,
    k_ref,
    v_ref,
    off_ref,
    hid_ref,
    gw_ref,
    ow_ref,
    o_ref,
    w_all,
    qh,
    kh,
    vh,
    offs,
    nout,
    ret,
    act,
    total,
    a_send,
    a_recv,
    r_send,
    r_recv,
    z_send,
    z_recv,
    x_send,
    x_recv,
    c_send,
    c_recv,
    loc_sem,
):
    s = lax.axis_index("sp")
    d = lax.axis_index("dp")
    rows = q_ref.shape[0]
    cols = q_ref.shape[1] // n_sp
    half = gw_ref.shape[0] // 2
    core, xi, yi = d % 2, (d // 2) % 2, d // 4
    d_c = d + 1 - 2 * core
    d_x = d + 2 - 4 * xi
    d_y = d + 4 - 8 * yi
    d_xy = d_x + 4 - 8 * yi
    low = s < 2
    order = [s, jnp.where(low, 1 - s, 5 - s), jnp.where(low, 2, 1), jnp.where(low, 3, 0)]
    peers = [(s + i) % n_sp for i in range(1, n_sp)]

    def cp(src, dst, ss, rs, dd, sd):
        return pltpu.make_async_remote_copy(
            src_ref=src,
            dst_ref=dst,
            send_sem=ss,
            recv_sem=rs,
            device_id=(sd, dd),
            device_id_type=pl.DeviceIdType.MESH,
        )

    local = []
    for w, ref in enumerate((gw_ref, ow_ref)):
        for hf in range(2):
            local.append(
                pltpu.make_async_copy(
                    ref.at[pl.ds(hf * half, half)], w_all.at[d, s, hf, w], loc_sem.at[2 * w + hf]
                )
            )
    mine = pl.ds(pl.multiple_of(s * cols, cols), cols)
    for i, (ref, dst) in enumerate(((q_ref, qh), (k_ref, kh), (v_ref, vh))):
        local.append(pltpu.make_async_copy(ref.at[:, mine], dst.at[s], loc_sem.at[4 + i]))
    local.append(pltpu.make_async_copy(off_ref.at[s], offs.at[s], loc_sem.at[7]))
    for c in local:
        c.start()

    barrier = pltpu.get_barrier_semaphore()
    friends = [(p, d) for p in peers] + [(s, d_x), (s, d_y), (s, d_c)]
    for ps, pd in friends:
        pl.semaphore_signal(
            barrier, inc=1, device_id=(ps, pd), device_id_type=pl.DeviceIdType.MESH
        )
    for c in local:
        c.wait()
    pl.semaphore_wait(barrier, len(friends))

    def x_copy(kind, r):
        b = order[r]
        if kind == 0:
            return cp(w_all.at[d, b], w_all.at[d, b], x_send.at[0, r], x_recv.at[0, r], d_x, s)
        if kind == 1:
            return cp(w_all.at[d, b], w_all.at[d, b], x_send.at[1, r], x_recv.at[1, r], d_y, s)
        if kind == 2:
            blk = w_all.at[d_y, b, 0]
            return cp(blk, blk, x_send.at[2, r], x_recv.at[2, r], d_x, s)
        blk = w_all.at[d_x, b, 1]
        return cp(blk, blk, x_send.at[3, r], x_recv.at[3, r], d_y, s)

    def c_copy(i, r):
        blk = w_all.at[(d, d_x, d_y, d_xy)[i], order[r]]
        return cp(blk, blk, c_send.at[i, r], c_recv.at[i, r], d_c, s)

    def z_copy(b, slot, to):
        blk = w_all.at[d, b]
        return cp(blk, blk, z_send.at[slot], z_recv.at[b], d, to)

    def z_arrival(r):
        b = order[r]
        return z_copy(b, 2 + r, s)

    def own_up_down():
        @pl.when(s < n_sp - 1)
        def _():
            z_copy(s, 0, s + 1).start()

        @pl.when(s > 0)
        def _():
            z_copy(s, 1, s - 1).start()

    middle = (s > 0) & (s < n_sp - 1)

    def forward_to(r):
        return jnp.where(order[r] < s, s + 1, s - 1)

    def stage1(r):
        if r > 0:
            z_arrival(r).wait_recv()

            @pl.when(middle)
            def _():
                z_copy(order[r], 2 + r, forward_to(r)).start()

        x_copy(0, r).start()
        x_copy(1, r).start()
        c_copy(0, r).start()

    def stage2(r):
        x_copy(1, r).wait_recv()
        x_copy(2, r).start()
        c_copy(2, r).start()
        x_copy(0, r).wait_recv()
        x_copy(3, r).start()
        c_copy(1, r).start()

    def stage3(r):
        x_copy(2, r).wait_recv()
        x_copy(3, r).wait_recv()
        c_copy(3, r).start()

    def a_copies(i):
        t = peers[i]
        theirs = pl.ds(pl.multiple_of(t * cols, cols), cols)
        out = []
        for n, (ref, dst) in enumerate(((q_ref, qh), (k_ref, kh), (v_ref, vh))):
            out.append(
                cp(ref.at[:, theirs], dst.at[s], a_send.at[n, i], a_recv.at[n, i], d, t)
            )
        out.append(cp(off_ref.at[t], offs.at[s], a_send.at[3, i], a_recv.at[3, i], d, t))
        return out

    def r_copy(i):
        t = peers[i]
        return cp(nout.at[t], ret.at[s], r_send.at[i], r_recv.at[i], d, t)

    def gate_block(r):
        b = order[r]
        for i in range(4):
            c_copy(i, r).wait_recv()

        def body(e, pre):
            lhs = hid_ref[:, pl.ds(pl.multiple_of(e * 2 * half, 2 * half), 2 * half)]
            rhs = w_all[e, b, :, 0].reshape(2 * half, cols)
            return pre + jnp.dot(lhs, rhs, preferred_element_type=f32)

        pre = lax.fori_loop(0, n_dp, body, jnp.zeros((rows, cols), f32), unroll=2)
        act[r] = pre / (1.0 + jnp.exp(-pre))

    def out_block(r):
        b = order[r]
        gated = (ret[b].astype(f32) * act[r]).astype(bf16)

        def body(e, carry):
            rhs = w_all[e, b, :, 1].reshape(cols, 2 * half)
            part = jnp.dot(gated, rhs, preferred_element_type=f32)
            if r == 0:
                total[e] = part
            elif r < n_sp - 1:
                total[e] += part
            else:
                where = pl.ds(pl.multiple_of(e * 2 * half, 2 * half), 2 * half)
                o_ref[:, where] = (total[e] + part).astype(bf16)
            return carry

        lax.fori_loop(0, n_dp, body, 0, unroll=2)

    lane = lax.broadcasted_iota(jnp.int32, (rows, 2 * head_size), 1)
    first = lane < head_size
    key_pos = lax.broadcasted_iota(jnp.int32, (rows, rows), 1)
    earlier = key_pos < lax.broadcasted_iota(jnp.int32, (rows, rows), 0)
    tri_row = lax.broadcasted_iota(jnp.int32, (2 * rows, rows), 0)
    tri_col = lax.broadcasted_iota(jnp.int32, (2 * rows, rows), 1)
    tri_row = jnp.where(tri_row >= rows, tri_row - rows, tri_row)
    tri = jnp.where(tri_row > tri_col, 1.0, 0.0).astype(bf16)

    def attend_pair(p):
        lanes = pl.ds(p * 2 * head_size, 2 * head_size)
        for i in range(n_sp):
            q_pair = qh[i, :, lanes]
            sums = []
            for h in range(2):
                q_one = jnp.where(first if h == 0 else ~first, q_pair, jnp.zeros_like(q_pair))
                carry = jnp.zeros((rows, 1), f32)
                acc = jnp.zeros((rows, 2 * head_size), f32)
                for j in range(i, -1, -1):
                    off = offs[j].astype(f32)[2 * p + h : 2 * p + h + 1, :] * log2_e
                    z = lax.dot_general(
                        q_one, kh[j, :, lanes], (((1,), (1,)), ((), ())),
                        preferred_element_type=f32,
                    )
                    z = z * (head_size ** (-0.5) * log2_e) - off
                    soft = jnp.log(1.0 + jnp.exp2(-jnp.abs(z))) * log2_e
                    keep = -(jnp.maximum(z, 0.0) + soft)
                    if j == i:
                        keep = jnp.where(earlier, keep, 0.0)
                    hi = keep.astype(bf16)
                    lo = (keep - hi.astype(f32)).astype(bf16)
                    later = jnp.dot(
                        jnp.concatenate([hi, lo], axis=1), tri, preferred_element_type=f32
                    )
                    wgt = jnp.exp2(jnp.minimum(z, 0.0) - soft + later + carry)
                    if j == i:
                        wgt = jnp.where(earlier, wgt, 0.0)
                    acc += jnp.dot(wgt.astype(bf16), vh[j, :, lanes], preferred_element_type=f32)
                    if j > 0:
                        carry += later[:, 0:1] + keep[:, 0:1]
                sums.append(acc)
            o = jnp.where(first, sums[0], sums[1])
            sq = o * o
            ms0 = jnp.sum(jnp.where(first, sq, 0.0), axis=1, keepdims=True)
            ms1 = jnp.sum(jnp.where(first, 0.0, sq), axis=1, keepdims=True)
            inv = jnp.where(
                first,
                lax.rsqrt(ms0 / head_size + eps_norm),
                lax.rsqrt(ms1 / head_size + eps_norm),
            )
            nout[i, :, lanes] = (o * inv).astype(bf16)

    pairs = cols // (2 * head_size)

    stage1(0)
    if QKV_FIRST:
        for i in range(n_sp - 1):
            for c in a_copies(i):
                c.start()
        own_up_down()
    else:
        own_up_down()
        for i in range(n_sp - 1):
            for c in a_copies(i):
                c.start()
    stage2(0)
    stage1(1)
    stage3(0)
    gate_block(0)
    stage2(1)
    for i in range(n_sp - 1):
        for c in a_copies(i):
            c.wait_recv()
    attend_pair(0)
    stage3(1)
    stage1(2)
    for p in range(1, pairs):
        attend_pair(p)
    for i in range(n_sp - 1):
        r_copy(i).start()
    ret[s] = nout[s]
    stage2(2)
    gate_block(1)
    stage1(3)
    stage3(2)
    stage2(3)
    gate_block(2)
    stage3(3)
    for i in range(n_sp - 1):
        r_copy(i).wait_recv()
    out_block(0)
    out_block(1)
    out_block(2)
    gate_block(3)
    out_block(3)

    for i in range(n_sp - 1):
        for c in a_copies(i):
            c.wait_send()
        r_copy(i).wait_send()
    for r in range(n_sp):
        for kind in range(4):
            x_copy(kind, r).wait_send()
            c_copy(kind, r).wait_send()

    @pl.when(s < n_sp - 1)
    def _():
        z_copy(s, 0, s + 1).wait_send()

    @pl.when(s > 0)
    def _():
        z_copy(s, 1, s - 1).wait_send()

    @pl.when(middle)
    def _():
        for r in range(1, n_sp):
            z_copy(order[r], 2 + r, forward_to(r)).wait_send()


def plane_shards(n_sp, n_dp, head_size, queries, key_rows, value_rows, break_offset, hidden_in, gate_weight, out_weight):
    rows, width = queries.shape[1:]
    heads_dev = break_offset.shape[2] // n_sp
    cols = width // n_sp
    depth = gate_weight.shape[0]
    offs = break_offset[0].T.reshape(n_sp, heads_dev, rows)
    vmem = pl.BlockSpec(memory_space=pltpu.VMEM)
    dma = pltpu.SemaphoreType.DMA
    mixed = pl.pallas_call(
        functools.partial(plane_kernel, n_sp, n_dp, head_size),
        out_shape=jax.ShapeDtypeStruct((rows, hidden_in.shape[2]), bf16),
        in_specs=[vmem] * 7,
        out_specs=vmem,
        scratch_shapes=[
            pltpu.VMEM((n_dp, n_sp, 2, 2, depth // 2, cols), bf16),
            pltpu.VMEM((n_sp, rows, cols), bf16),
            pltpu.VMEM((n_sp, rows, cols), bf16),
            pltpu.VMEM((n_sp, rows, cols), bf16),
            pltpu.VMEM((n_sp, heads_dev, rows), bf16),
            pltpu.VMEM((n_sp, rows, cols), bf16),
            pltpu.VMEM((n_sp, rows, cols), bf16),
            pltpu.VMEM((n_sp, rows, cols), f32),
            pltpu.VMEM((n_dp, rows, cols), f32),
            dma((4, n_sp - 1)),
            dma((4, n_sp - 1)),
            dma((n_sp - 1,)),
            dma((n_sp - 1,)),
            dma((2 + n_sp,)),
            dma((n_sp,)),
            dma((4, n_sp)),
            dma((4, n_sp)),
            dma((4, n_sp)),
            dma((4, n_sp)),
            dma((8,)),
        ],
        compiler_params=pltpu.CompilerParams(
            collective_id=0, has_side_effects=True, vmem_limit_bytes=60 * 1024 * 1024
        ),
    )(queries[0], key_rows[0], value_rows[0], offs, hidden_in[0], gate_weight, out_weight)
    return mixed[None]


def planned(mesh, shards_general):
    n_sp, n_dp = mesh.shape["sp"], mesh.shape["dp"]

    def run(*local):
        queries, break_offset, gate_weight, out_weight = local[0], local[3], local[5], local[6]
        head_size = queries.shape[2] // break_offset.shape[2]
        cols = queries.shape[2] // n_sp
        if (
            n_sp == 4
            and n_dp == 8
            and queries.shape[0] == 1
            and queries.shape[1] == 128
            and 2 * head_size == 128
            and cols % 128 == 0
            and gate_weight.shape == out_weight.shape == (cols, cols)
        ):
            return plane_shards(n_sp, n_dp, head_size, *local)
        return shards_general(*local)

    return run


def solution(mesh):
    return jax.shard_map(
        planned(mesh, shards),
        mesh=mesh,
        in_specs=(
            P("dp", "sp", None),
            P("dp", "sp", None),
            P("dp", "sp", None),
            P("dp", "sp", None),
            P("dp", "sp", None),
            P("dp", "sp"),
            P("sp", "dp"),
        ),
        out_specs=P("dp", "sp", None),
        check_vma=False,
    )
```

```python
import functools
import math
import jax
import jax.numpy as jnp
from jax import lax
from jax.experimental import pallas as pl
from jax.experimental.pallas import tpu as pltpu
from jax.sharding import PartitionSpec as P

eps_norm = 1e-05


def stick_blocks(head_queries, head_keys, head_values, head_offsets):
    groups, length, head_size = head_queries.shape
    block_rows = min(512, length)
    block_count = length // block_rows
    score_scale = head_size ** (-0.5)
    query_blocks = head_queries.reshape(groups, block_count, block_rows, head_size)

    def one_block(block_index):
        query_block = lax.dynamic_index_in_dim(query_blocks, block_index, 1, keepdims=False)
        query_pos = block_index * block_rows + jnp.arange(block_rows, dtype=jnp.int32)

        def key_step(step_turn, carry):
            running, carried = carry
            key_first = (block_index - step_turn) * block_rows
            key_block = lax.dynamic_slice_in_dim(head_keys, key_first, block_rows, 1)
            value_block = lax.dynamic_slice_in_dim(head_values, key_first, block_rows, 1)
            offset_block = lax.dynamic_slice_in_dim(head_offsets, key_first, block_rows, 1)
            scores = jnp.einsum(
                "gqd,gkd->gqk", query_block, key_block, preferred_element_type=jnp.float32
            )
            scores = scores * score_scale - offset_block[:, None, :]
            key_pos = key_first + jnp.arange(block_rows, dtype=jnp.int32)
            earlier = key_pos[None, :] < query_pos[:, None]
            keep_log = jnp.where(earlier, jax.nn.log_sigmoid(-scores), 0.0)
            later_sum = lax.cumsum(keep_log, axis=2, reverse=True) - keep_log + carried
            weights = jnp.where(
                earlier, jnp.exp(jax.nn.log_sigmoid(scores) + later_sum), 0.0
            ).astype(jnp.bfloat16)
            running = running + jnp.einsum(
                "gqk,gkd->gqd", weights, value_block, preferred_element_type=jnp.float32
            )
            carried = carried + jnp.sum(keep_log, axis=2, keepdims=True)
            return (running, carried)

        start_carry = (
            jnp.zeros((groups, block_rows, head_size), jnp.float32),
            jnp.zeros((groups, block_rows, 1), jnp.float32),
        )
        running, carried = lax.fori_loop(0, block_index + 1, key_step, start_carry)
        return running

    outputs = lax.map(one_block, jnp.arange(block_count, dtype=jnp.int32))
    return outputs.transpose(1, 0, 2, 3).reshape(groups, length, head_size)


def attend(pieces):
    head_queries, head_keys, head_values, head_offsets = pieces
    item_count, length, feature_count = head_queries.shape
    heads_dev = head_offsets.shape[2]
    head_size = feature_count // heads_dev

    def split_heads(array):
        return (
            array.reshape(item_count, length, heads_dev, head_size)
            .transpose(0, 2, 1, 3)
            .reshape(item_count * heads_dev, length, head_size)
        )

    offsets = (
        head_offsets.transpose(0, 2, 1).reshape(item_count * heads_dev, length).astype(jnp.float32)
    )
    heads_out = stick_blocks(
        split_heads(head_queries), split_heads(head_keys), split_heads(head_values), offsets
    )
    mean_sq = jnp.mean(heads_out * heads_out, axis=2, keepdims=True)
    normed = (heads_out * lax.rsqrt(mean_sq + eps_norm)).astype(jnp.bfloat16)
    return (
        normed.reshape(item_count, heads_dev, length, head_size)
        .transpose(0, 2, 1, 3)
        .reshape(item_count, length, feature_count)
    )


def shards(queries, key_rows, value_rows, break_offset, hidden_in, gate_weight, out_weight):
    tokens = hidden_in[0]
    gate_rows, out_cols = (
        lax.all_gather(gate_weight, "sp", axis=1, tiled=True),
        lax.all_gather(out_weight, "sp", axis=0, tiled=True),
    )
    gate_pre = jnp.dot(
        tokens,
        lax.all_gather(gate_rows, "dp", axis=0, tiled=True),
        preferred_element_type=jnp.float32,
    )
    gate_act = jax.nn.silu(gate_pre)
    normed = attend(
        (
            lax.all_to_all(queries, "sp", split_axis=2, concat_axis=1, tiled=True),
            lax.all_to_all(key_rows, "sp", split_axis=2, concat_axis=1, tiled=True),
            lax.all_to_all(value_rows, "sp", split_axis=2, concat_axis=1, tiled=True),
            lax.all_to_all(break_offset, "sp", split_axis=2, concat_axis=1, tiled=True),
        )
    )
    returned = lax.all_to_all(normed, "sp", split_axis=1, concat_axis=2, tiled=True)
    gated_rows = (returned[0].astype(jnp.float32) * gate_act).astype(jnp.bfloat16)
    mixed_rows = jnp.dot(
        gated_rows,
        lax.all_gather(out_cols, "dp", axis=1, tiled=True),
        preferred_element_type=jnp.float32,
    )
    return mixed_rows.astype(jnp.bfloat16)[None]


log2_e = math.log2(math.e)
f32, bf16 = jnp.float32, jnp.bfloat16


def plane_kernel(
    n_sp,
    n_dp,
    head_size,
    q_ref,
    k_ref,
    v_ref,
    off_ref,
    hid_ref,
    gw_ref,
    ow_ref,
    o_ref,
    hid,
    w_all,
    qh,
    kh,
    vh,
    offs,
    nout,
    ret,
    act,
    total,
    a_send,
    a_recv,
    r_send,
    r_recv,
    z_send,
    z_recv,
    x_send,
    x_recv,
    c_send,
    c_recv,
    loc_sem,
):
    s = lax.axis_index("sp")
    d = lax.axis_index("dp")
    rows = q_ref.shape[0]
    cols = q_ref.shape[1] // n_sp
    half = gw_ref.shape[0] // 2
    core, xi, yi = d % 2, (d // 2) % 2, d // 4
    d_c = d + 1 - 2 * core
    d_x = d + 2 - 4 * xi
    d_y = d + 4 - 8 * yi
    d_xy = d_x + 4 - 8 * yi
    low = s < 2
    order = [s, jnp.where(low, 1 - s, 5 - s), jnp.where(low, 2, 1), jnp.where(low, 3, 0)]
    peers = [(s + i) % n_sp for i in range(1, n_sp)]

    def cp(src, dst, ss, rs, dd, sd):
        return pltpu.make_async_remote_copy(
            src_ref=src,
            dst_ref=dst,
            send_sem=ss,
            recv_sem=rs,
            device_id=(sd, dd),
            device_id_type=pl.DeviceIdType.MESH,
        )

    own = []
    for w, ref in enumerate((gw_ref, ow_ref)):
        for hf in range(2):
            own.append(
                pltpu.make_async_copy(
                    ref.at[pl.ds(hf * half, half)], w_all.at[w, d, s, hf], loc_sem.at[2 * w + hf]
                )
            )
    mine = pl.ds(pl.multiple_of(s * cols, cols), cols)
    local = []
    for i, (ref, dst) in enumerate(((q_ref, qh), (k_ref, kh), (v_ref, vh))):
        local.append(pltpu.make_async_copy(ref.at[:, mine], dst.at[s], loc_sem.at[4 + i]))
    local.append(pltpu.make_async_copy(off_ref.at[s], offs.at[s], loc_sem.at[7]))
    local.append(pltpu.make_async_copy(hid_ref, hid, loc_sem.at[8]))
    for c in own + local:
        c.start()

    barrier = pltpu.get_barrier_semaphore()
    friends = [(p, d) for p in peers] + [(s, d_x), (s, d_y), (s, d_c)]
    for ps, pd in friends:
        pl.semaphore_signal(
            barrier, inc=1, device_id=(ps, pd), device_id_type=pl.DeviceIdType.MESH
        )
    for c in own:
        c.wait()
    pl.semaphore_wait(barrier, len(friends))

    def x_copy(kind, n):
        w, b = n % 2, order[n // 2]
        src = (
            w_all.at[w, d, b],
            w_all.at[w, d, b],
            w_all.at[w, d_y, b, 0],
            w_all.at[w, d_x, b, 1],
        )[kind]
        return cp(
            src, src, x_send.at[kind, n], x_recv.at[kind, n], d_x if kind % 2 == 0 else d_y, s
        )

    def c_copy(i, n):
        blk = w_all.at[n % 2, (d, d_x, d_y, d_xy)[i], order[n // 2]]
        return cp(blk, blk, c_send.at[i, n], c_recv.at[i, n], d_c, s)

    def z_copy(w, b, slot, to):
        blk = w_all.at[w, d, b]
        return cp(blk, blk, z_send.at[w, slot], z_recv.at[w, b], d, to)

    def own_up_down(w):
        @pl.when(s < n_sp - 1)
        def _():
            z_copy(w, s, 0, s + 1).start()

        @pl.when(s > 0)
        def _():
            z_copy(w, s, 1, s - 1).start()

    middle = (s > 0) & (s < n_sp - 1)

    def forward_to(r):
        return jnp.where(order[r] < s, s + 1, s - 1)

    def stage1(n):
        w, r = n % 2, n // 2
        if r > 0:
            z_copy(w, order[r], 2 + r, s).wait_recv()

            @pl.when(middle)
            def _():
                z_copy(w, order[r], 2 + r, forward_to(r)).start()

        x_copy(0, n).start()
        x_copy(1, n).start()
        c_copy(0, n).start()

    def stage2(n):
        x_copy(1, n).wait_recv()
        x_copy(2, n).start()
        c_copy(2, n).start()
        x_copy(0, n).wait_recv()
        x_copy(3, n).start()
        c_copy(1, n).start()

    def stage3(n):
        x_copy(2, n).wait_recv()
        x_copy(3, n).wait_recv()
        c_copy(3, n).start()

    def a_copies(t, source):
        theirs = pl.ds(pl.multiple_of(t * cols, cols), cols)
        out = []
        for n, (ref, dst) in enumerate(((q_ref, qh), (k_ref, kh), (v_ref, vh))):
            out.append(
                cp(ref.at[:, theirs], dst.at[source], a_send.at[n, t], a_recv.at[n, source], d, t)
            )
        out.append(
            cp(off_ref.at[t], offs.at[source], a_send.at[3, t], a_recv.at[3, source], d, t)
        )
        return out

    def r_copy(t, source):
        return cp(nout.at[t], ret.at[source], r_send.at[t], r_recv.at[source], d, t)

    def gate_block(r):
        b = order[r]
        for i in range(4):
            c_copy(i, 2 * r).wait_recv()

        def body(e, pre):
            lhs = hid[:, pl.ds(pl.multiple_of(e * 2 * half, 2 * half), 2 * half)]
            rhs = w_all[0, e, b].reshape(2 * half, cols)
            return pre + jnp.dot(lhs, rhs, preferred_element_type=f32)

        pre = lax.fori_loop(0, n_dp, body, jnp.zeros((rows, cols), f32), unroll=2)
        act[r] = pre / (1.0 + jnp.exp(-pre))

    def out_block(r):
        b = order[r]
        for i in range(4):
            c_copy(i, 2 * r + 1).wait_recv()
        gated = (ret[b].astype(f32) * act[r]).astype(bf16)

        def body(e, carry):
            rhs = w_all[1, e, b].reshape(cols, 2 * half)
            part = jnp.dot(gated, rhs, preferred_element_type=f32)
            if r == 0:
                total[e] = part
            elif r < n_sp - 1:
                total[e] += part
            else:
                where = pl.ds(pl.multiple_of(e * 2 * half, 2 * half), 2 * half)
                o_ref[:, where] = (total[e] + part).astype(bf16)
            return carry

        lax.fori_loop(0, n_dp, body, 0, unroll=2)

    lane = lax.broadcasted_iota(jnp.int32, (rows, 2 * head_size), 1)
    first = lane < head_size
    key_pos = lax.broadcasted_iota(jnp.int32, (rows, rows), 1)
    earlier = key_pos < lax.broadcasted_iota(jnp.int32, (rows, rows), 0)
    tri_row = lax.broadcasted_iota(jnp.int32, (2 * rows, rows), 0)
    tri_col = lax.broadcasted_iota(jnp.int32, (2 * rows, rows), 1)
    tri_row = jnp.where(tri_row >= rows, tri_row - rows, tri_row)
    tri = jnp.where(tri_row > tri_col, 1.0, 0.0).astype(bf16)

    def attend(i, p):
        lanes = pl.ds(p * 2 * head_size, 2 * head_size)
        if True:
            q_pair = qh[i, :, lanes]
            sums = []
            for h in range(2):
                q_one = jnp.where(first if h == 0 else ~first, q_pair, jnp.zeros_like(q_pair))
                carry = jnp.zeros((rows, 1), f32)
                acc = jnp.zeros((rows, 2 * head_size), f32)
                for j in range(i, -1, -1):
                    off = offs[j].astype(f32)[2 * p + h : 2 * p + h + 1, :] * log2_e
                    z = lax.dot_general(
                        q_one, kh[j, :, lanes], (((1,), (1,)), ((), ())),
                        preferred_element_type=f32,
                    )
                    z = z * (head_size ** (-0.5) * log2_e) - off
                    soft = jnp.log(1.0 + jnp.exp2(-jnp.abs(z))) * log2_e
                    keep = -(jnp.maximum(z, 0.0) + soft)
                    if j == i:
                        keep = jnp.where(earlier, keep, 0.0)
                    hi = keep.astype(bf16)
                    lo = (keep - hi.astype(f32)).astype(bf16)
                    later = jnp.dot(
                        jnp.concatenate([hi, lo], axis=1), tri, preferred_element_type=f32
                    )
                    wgt = jnp.exp2(jnp.minimum(z, 0.0) - soft + later + carry)
                    if j == i:
                        wgt = jnp.where(earlier, wgt, 0.0)
                    acc += jnp.dot(wgt.astype(bf16), vh[j, :, lanes], preferred_element_type=f32)
                    if j > 0:
                        carry += later[:, 0:1] + keep[:, 0:1]
                sums.append(acc)
            o = jnp.where(first, sums[0], sums[1])
            sq = o * o
            ms0 = jnp.sum(jnp.where(first, sq, 0.0), axis=1, keepdims=True)
            ms1 = jnp.sum(jnp.where(first, 0.0, sq), axis=1, keepdims=True)
            inv = jnp.where(
                first,
                lax.rsqrt(ms0 / head_size + eps_norm),
                lax.rsqrt(ms1 / head_size + eps_norm),
            )
            nout[i, :, lanes] = (o * inv).astype(bf16)

    pairs = cols // (2 * head_size)

    def attend_row(i, between):
        @pl.when(s != i)
        def _():
            for c in a_copies(s, i):
                c.wait_recv()

        for p in range(pairs):
            attend(i, p)
            for act_on in between[p : p + 1]:
                for stage, n in act_on:
                    stage(n)

        @pl.when(s != i)
        def _():
            r_copy(i, s).start()

        @pl.when(s == i)
        def _():
            ret[i] = nout[i]

    stage1(0)
    own_up_down(0)
    stage1(1)
    own_up_down(1)
    for t in peers:
        for c in a_copies(t, s):
            c.start()
    for c in local:
        c.wait()
    for stage, n in (
        (stage2, 0), (stage1, 2), (stage2, 1), (stage1, 3), (stage3, 0), (stage3, 1),
        (gate_block, 0), (stage2, 2), (stage2, 3), (stage3, 2), (gate_block, 1), (stage3, 3),
        (stage1, 4),
    ):
        stage(n)
    attend_row(0, ((), ((stage1, 5),)))
    attend_row(1, ((), ((stage2, 4), (stage2, 5))))
    attend_row(2, (((stage1, 6),), ((stage3, 4), (stage1, 7))))
    attend_row(3, (((stage3, 5), (stage2, 6)), ((stage2, 7),)))
    gate_block(2)
    stage3(6)
    stage3(7)
    for t in peers:
        r_copy(s, t).wait_recv()
    out_block(0)
    out_block(1)
    out_block(2)
    gate_block(3)
    out_block(3)
    for t in peers:
        for c in a_copies(t, s):
            c.wait_send()
        r_copy(t, s).wait_send()
    for n in range(2 * n_sp):
        for kind in range(4):
            x_copy(kind, n).wait_send()
            c_copy(kind, n).wait_send()
    for w in range(2):

        @pl.when(s < n_sp - 1)
        def _():
            z_copy(w, s, 0, s + 1).wait_send()

        @pl.when(s > 0)
        def _():
            z_copy(w, s, 1, s - 1).wait_send()

        @pl.when(middle)
        def _():
            for r in range(1, n_sp):
                z_copy(w, order[r], 2 + r, forward_to(r)).wait_send()


def plane_shards(n_sp, n_dp, head_size, queries, key_rows, value_rows, break_offset, hidden_in, gate_weight, out_weight):
    rows, width = queries.shape[1:]
    heads_dev = break_offset.shape[2] // n_sp
    cols = width // n_sp
    depth = gate_weight.shape[0]
    offs = break_offset[0].T.reshape(n_sp, heads_dev, rows)
    vmem = pl.BlockSpec(memory_space=pltpu.VMEM)
    dma = pltpu.SemaphoreType.DMA
    mixed = pl.pallas_call(
        functools.partial(plane_kernel, n_sp, n_dp, head_size),
        out_shape=pltpu.VMEM((rows, hidden_in.shape[2]), bf16),
        in_specs=[pl.BlockSpec(memory_space=pl.ANY)] * 7,
        out_specs=vmem,
        scratch_shapes=[
            pltpu.VMEM((rows, depth * n_dp), bf16),
            pltpu.VMEM((2, n_dp, n_sp, 2, depth // 2, cols), bf16),
            pltpu.VMEM((n_sp, rows, cols), bf16),
            pltpu.VMEM((n_sp, rows, cols), bf16),
            pltpu.VMEM((n_sp, rows, cols), bf16),
            pltpu.VMEM((n_sp, heads_dev, rows), bf16),
            pltpu.VMEM((n_sp, rows, cols), bf16),
            pltpu.VMEM((n_sp, rows, cols), bf16),
            pltpu.VMEM((n_sp, rows, cols), f32),
            pltpu.VMEM((n_dp, rows, cols), f32),
            dma((4, n_sp)),
            dma((4, n_sp)),
            dma((n_sp,)),
            dma((n_sp,)),
            dma((2, 2 + n_sp)),
            dma((2, n_sp)),
            dma((4, 2 * n_sp)),
            dma((4, 2 * n_sp)),
            dma((4, 2 * n_sp)),
            dma((4, 2 * n_sp)),
            dma((9,)),
        ],
        compiler_params=pltpu.CompilerParams(
            collective_id=0, has_side_effects=True, vmem_limit_bytes=60 * 1024 * 1024
        ),
    )(queries[0], key_rows[0], value_rows[0], offs, hidden_in[0], gate_weight, out_weight)
    return mixed[None]


def planned(mesh, shards_general):
    n_sp, n_dp = mesh.shape["sp"], mesh.shape["dp"]

    def run(*local):
        queries, break_offset, gate_weight, out_weight = local[0], local[3], local[5], local[6]
        head_size = queries.shape[2] // break_offset.shape[2]
        cols = queries.shape[2] // n_sp
        if (
            n_sp == 4
            and n_dp == 8
            and queries.shape[0] == 1
            and queries.shape[1] == 128
            and 2 * head_size == 128
            and cols % 128 == 0
            and gate_weight.shape == out_weight.shape == (cols, cols)
        ):
            return plane_shards(n_sp, n_dp, head_size, *local)
        return shards_general(*local)

    return run


def solution(mesh):
    return jax.shard_map(
        planned(mesh, shards),
        mesh=mesh,
        in_specs=(
            P("dp", "sp", None),
            P("dp", "sp", None),
            P("dp", "sp", None),
            P("dp", "sp", None),
            P("dp", "sp", None),
            P("dp", "sp"),
            P("sp", "dp"),
        ),
        out_specs=P("dp", "sp", None),
        check_vma=False,
    )
```

```python
import functools
import math
import jax
import jax.numpy as jnp
from jax import lax
from jax.experimental import pallas as pl
from jax.experimental.pallas import tpu as pltpu
from jax.sharding import PartitionSpec as P

eps_norm = 1e-05


def stick_blocks(head_queries, head_keys, head_values, head_offsets):
    groups, length, head_size = head_queries.shape
    block_rows = min(512, length)
    block_count = length // block_rows
    score_scale = head_size ** (-0.5)
    query_blocks = head_queries.reshape(groups, block_count, block_rows, head_size)

    def one_block(block_index):
        query_block = lax.dynamic_index_in_dim(query_blocks, block_index, 1, keepdims=False)
        query_pos = block_index * block_rows + jnp.arange(block_rows, dtype=jnp.int32)

        def key_step(step_turn, carry):
            running, carried = carry
            key_first = (block_index - step_turn) * block_rows
            key_block = lax.dynamic_slice_in_dim(head_keys, key_first, block_rows, 1)
            value_block = lax.dynamic_slice_in_dim(head_values, key_first, block_rows, 1)
            offset_block = lax.dynamic_slice_in_dim(head_offsets, key_first, block_rows, 1)
            scores = jnp.einsum(
                "gqd,gkd->gqk", query_block, key_block, preferred_element_type=jnp.float32
            )
            scores = scores * score_scale - offset_block[:, None, :]
            key_pos = key_first + jnp.arange(block_rows, dtype=jnp.int32)
            earlier = key_pos[None, :] < query_pos[:, None]
            keep_log = jnp.where(earlier, jax.nn.log_sigmoid(-scores), 0.0)
            later_sum = lax.cumsum(keep_log, axis=2, reverse=True) - keep_log + carried
            weights = jnp.where(
                earlier, jnp.exp(jax.nn.log_sigmoid(scores) + later_sum), 0.0
            ).astype(jnp.bfloat16)
            running = running + jnp.einsum(
                "gqk,gkd->gqd", weights, value_block, preferred_element_type=jnp.float32
            )
            carried = carried + jnp.sum(keep_log, axis=2, keepdims=True)
            return (running, carried)

        start_carry = (
            jnp.zeros((groups, block_rows, head_size), jnp.float32),
            jnp.zeros((groups, block_rows, 1), jnp.float32),
        )
        running, carried = lax.fori_loop(0, block_index + 1, key_step, start_carry)
        return running

    outputs = lax.map(one_block, jnp.arange(block_count, dtype=jnp.int32))
    return outputs.transpose(1, 0, 2, 3).reshape(groups, length, head_size)


def attend(pieces):
    head_queries, head_keys, head_values, head_offsets = pieces
    item_count, length, feature_count = head_queries.shape
    heads_dev = head_offsets.shape[2]
    head_size = feature_count // heads_dev

    def split_heads(array):
        return (
            array.reshape(item_count, length, heads_dev, head_size)
            .transpose(0, 2, 1, 3)
            .reshape(item_count * heads_dev, length, head_size)
        )

    offsets = (
        head_offsets.transpose(0, 2, 1).reshape(item_count * heads_dev, length).astype(jnp.float32)
    )
    heads_out = stick_blocks(
        split_heads(head_queries), split_heads(head_keys), split_heads(head_values), offsets
    )
    mean_sq = jnp.mean(heads_out * heads_out, axis=2, keepdims=True)
    normed = (heads_out * lax.rsqrt(mean_sq + eps_norm)).astype(jnp.bfloat16)
    return (
        normed.reshape(item_count, heads_dev, length, head_size)
        .transpose(0, 2, 1, 3)
        .reshape(item_count, length, feature_count)
    )


def shards(queries, key_rows, value_rows, break_offset, hidden_in, gate_weight, out_weight):
    tokens = hidden_in[0]
    gate_rows, out_cols = (
        lax.all_gather(gate_weight, "sp", axis=1, tiled=True),
        lax.all_gather(out_weight, "sp", axis=0, tiled=True),
    )
    gate_pre = jnp.dot(
        tokens,
        lax.all_gather(gate_rows, "dp", axis=0, tiled=True),
        preferred_element_type=jnp.float32,
    )
    gate_act = jax.nn.silu(gate_pre)
    normed = attend(
        (
            lax.all_to_all(queries, "sp", split_axis=2, concat_axis=1, tiled=True),
            lax.all_to_all(key_rows, "sp", split_axis=2, concat_axis=1, tiled=True),
            lax.all_to_all(value_rows, "sp", split_axis=2, concat_axis=1, tiled=True),
            lax.all_to_all(break_offset, "sp", split_axis=2, concat_axis=1, tiled=True),
        )
    )
    returned = lax.all_to_all(normed, "sp", split_axis=1, concat_axis=2, tiled=True)
    gated_rows = (returned[0].astype(jnp.float32) * gate_act).astype(jnp.bfloat16)
    mixed_rows = jnp.dot(
        gated_rows,
        lax.all_gather(out_cols, "dp", axis=1, tiled=True),
        preferred_element_type=jnp.float32,
    )
    return mixed_rows.astype(jnp.bfloat16)[None]


log2_e = math.log2(math.e)
f32, bf16 = jnp.float32, jnp.bfloat16


def plane_kernel(
    n_sp,
    n_dp,
    head_size,
    q_ref,
    k_ref,
    v_ref,
    off_ref,
    hid_ref,
    gw_ref,
    ow_ref,
    o_ref,
    hid,
    w_all,
    qh,
    kh,
    vh,
    offs,
    nout,
    ret,
    act,
    total,
    a_send,
    a_recv,
    r_send,
    r_recv,
    z_send,
    z_recv,
    x_send,
    x_recv,
    c_send,
    c_recv,
    loc_sem,
    hx,
    p_out,
    p_in,
    h_send,
    h_recv,
    p_send,
    p_recv,
):
    s = lax.axis_index("sp")
    d = lax.axis_index("dp")
    rows = q_ref.shape[0]
    cols = q_ref.shape[1] // n_sp
    half = gw_ref.shape[0] // 2
    core, xi, yi = d % 2, (d // 2) % 2, d // 4
    d_c = d + 1 - 2 * core
    d_x = d + 2 - 4 * xi
    d_y = d + 4 - 8 * yi
    d_xy = d_x + 4 - 8 * yi
    low = s < 2
    order = [s, jnp.where(low, 1 - s, 5 - s), jnp.where(low, 2, 1), jnp.where(low, 3, 0)]
    peers = [(s + i) % n_sp for i in range(1, n_sp)]

    def cp(src, dst, ss, rs, dd, sd):
        return pltpu.make_async_remote_copy(
            src_ref=src,
            dst_ref=dst,
            send_sem=ss,
            recv_sem=rs,
            device_id=(sd, dd),
            device_id_type=pl.DeviceIdType.MESH,
        )

    own = []
    for w, ref in enumerate((gw_ref, ow_ref)):
        for hf in range(2):
            own.append(
                pltpu.make_async_copy(
                    ref.at[pl.ds(hf * half, half)], w_all.at[w, d, s, hf], loc_sem.at[2 * w + hf]
                )
            )
    mine = pl.ds(pl.multiple_of(s * cols, cols), cols)
    local = []
    for i, (ref, dst) in enumerate(((q_ref, qh), (k_ref, kh), (v_ref, vh))):
        local.append(pltpu.make_async_copy(ref.at[:, mine], dst.at[s], loc_sem.at[4 + i]))
    local.append(pltpu.make_async_copy(off_ref.at[s], offs.at[s], loc_sem.at[7]))
    local.append(pltpu.make_async_copy(hid_ref, hid, loc_sem.at[8]))
    for c in own + local:
        c.start()

    barrier = pltpu.get_barrier_semaphore()
    friends = [(p, d) for p in peers] + [(s, d_x), (s, d_y), (s, d_c)]
    for ps, pd in friends:
        pl.semaphore_signal(
            barrier, inc=1, device_id=(ps, pd), device_id_type=pl.DeviceIdType.MESH
        )
    for c in own:
        c.wait()
    pl.semaphore_wait(barrier, len(friends))

    def x_copy(kind, n):
        w, b = n % 2, order[n // 2]
        src = (
            w_all.at[w, d, b],
            w_all.at[w, d, b],
            w_all.at[w, d_y, b, 0],
            w_all.at[w, d_x, b, 1],
        )[kind]
        return cp(
            src, src, x_send.at[kind, n], x_recv.at[kind, n], d_x if kind % 2 == 0 else d_y, s
        )

    def c_copy(i, n):
        blk = w_all.at[n % 2, (d, d_x, d_y, d_xy)[i], order[n // 2]]
        return cp(blk, blk, c_send.at[i, n], c_recv.at[i, n], d_c, s)

    def z_copy(w, b, slot, to):
        blk = w_all.at[w, d, b]
        return cp(blk, blk, z_send.at[w, slot], z_recv.at[w, b], d, to)

    def own_up_down(w):
        @pl.when(s < n_sp - 1)
        def _():
            z_copy(w, s, 0, s + 1).start()

        @pl.when(s > 0)
        def _():
            z_copy(w, s, 1, s - 1).start()

    middle = (s > 0) & (s < n_sp - 1)

    def forward_to(r):
        return jnp.where(order[r] < s, s + 1, s - 1)

    def stage1(n):
        w, r = n % 2, n // 2
        if r > 0:
            z_copy(w, order[r], 2 + r, s).wait_recv()

            @pl.when(middle)
            def _():
                z_copy(w, order[r], 2 + r, forward_to(r)).start()

        if w == 1:
            x_copy(0, n).start()
        x_copy(1, n).start()
        c_copy(0, n).start()

    def stage2(n):
        x_copy(1, n).wait_recv()
        if n % 2 == 0:
            c_copy(2, n).start()
            return
        x_copy(2, n).start()
        c_copy(2, n).start()
        x_copy(0, n).wait_recv()
        x_copy(3, n).start()
        c_copy(1, n).start()

    def stage3(n):
        if n % 2 == 0:
            return
        x_copy(2, n).wait_recv()
        x_copy(3, n).wait_recv()
        c_copy(3, n).start()

    def a_copies(t, source):
        theirs = pl.ds(pl.multiple_of(t * cols, cols), cols)
        out = []
        for n, (ref, dst) in enumerate(((q_ref, qh), (k_ref, kh), (v_ref, vh))):
            out.append(
                cp(ref.at[:, theirs], dst.at[source], a_send.at[n, t], a_recv.at[n, source], d, t)
            )
        out.append(
            cp(off_ref.at[t], offs.at[source], a_send.at[3, t], a_recv.at[3, source], d, t)
        )
        return out

    def r_copy(t, source):
        return cp(nout.at[t], ret.at[source], r_send.at[t], r_recv.at[source], d, t)

    def h_copy(yy):
        theirs = pl.ds(pl.multiple_of((yy * 4 + (1 - xi) * 2) * 2 * half, 4 * half), 4 * half)
        return cp(hid_ref.at[:, theirs], hx.at[yy], h_send.at[yy], h_recv.at[yy], d_x, s)

    def p_copy(r):
        return cp(p_out.at[r], p_in.at[r], p_send.at[r], p_recv.at[r], d_x, s)

    def gate_block(r):
        b = order[r]
        c_copy(0, 2 * r).wait_recv()
        c_copy(2, 2 * r).wait_recv()
        if r == 0:
            h_copy(0).wait_recv()
            h_copy(1).wait_recv()
        pre = jnp.zeros((2 * rows, cols), f32)
        for yy in range(2):
            for cc in range(2):
                e = yy * 4 + xi * 2 + cc
                lhs = hid[:, pl.ds(pl.multiple_of(e * 2 * half, 2 * half), 2 * half)]
                other = hx[yy, :, cc * 2 * half : (cc + 1) * 2 * half]
                rhs = w_all[0, e, b].reshape(2 * half, cols)
                pre += jnp.dot(
                    jnp.concatenate([lhs, other], axis=0), rhs, preferred_element_type=f32
                )
        act[r] = pre[:rows]
        p_out[r] = pre[rows:].astype(bf16)
        p_copy(r).start()

    def out_block(r):
        b = order[r]
        for i in range(4):
            c_copy(i, 2 * r + 1).wait_recv()
        p_copy(r).wait_recv()
        pre = act[r] + p_in[r].astype(f32)
        gated = (ret[b].astype(f32) * (pre / (1.0 + jnp.exp(-pre)))).astype(bf16)

        def body(e, carry):
            rhs = w_all[1, e, b].reshape(cols, 2 * half)
            part = jnp.dot(gated, rhs, preferred_element_type=f32)
            if r == 0:
                total[e] = part
            elif r < n_sp - 1:
                total[e] += part
            else:
                where = pl.ds(pl.multiple_of(e * 2 * half, 2 * half), 2 * half)
                o_ref[:, where] = (total[e] + part).astype(bf16)
            return carry

        lax.fori_loop(0, n_dp, body, 0, unroll=2)

    lane = lax.broadcasted_iota(jnp.int32, (rows, 2 * head_size), 1)
    first = lane < head_size
    key_pos = lax.broadcasted_iota(jnp.int32, (rows, rows), 1)
    earlier = key_pos < lax.broadcasted_iota(jnp.int32, (rows, rows), 0)
    tri_row = lax.broadcasted_iota(jnp.int32, (2 * rows, rows), 0)
    tri_col = lax.broadcasted_iota(jnp.int32, (2 * rows, rows), 1)
    tri_row = jnp.where(tri_row >= rows, tri_row - rows, tri_row)
    tri = jnp.where(tri_row > tri_col, 1.0, 0.0).astype(bf16)

    def attend(i, p):
        lanes = pl.ds(p * 2 * head_size, 2 * head_size)
        if True:
            q_pair = qh[i, :, lanes]
            sums = []
            for h in range(2):
                q_one = jnp.where(first if h == 0 else ~first, q_pair, jnp.zeros_like(q_pair))
                carry = jnp.zeros((rows, 1), f32)
                acc = jnp.zeros((rows, 2 * head_size), f32)
                for j in range(i, -1, -1):
                    off = offs[j].astype(f32)[2 * p + h : 2 * p + h + 1, :] * log2_e
                    z = lax.dot_general(
                        q_one, kh[j, :, lanes], (((1,), (1,)), ((), ())),
                        preferred_element_type=f32,
                    )
                    z = z * (head_size ** (-0.5) * log2_e) - off
                    soft = jnp.log(1.0 + jnp.exp2(-jnp.abs(z))) * log2_e
                    keep = -(jnp.maximum(z, 0.0) + soft)
                    if j == i:
                        keep = jnp.where(earlier, keep, 0.0)
                    hi = keep.astype(bf16)
                    lo = (keep - hi.astype(f32)).astype(bf16)
                    later = jnp.dot(
                        jnp.concatenate([hi, lo], axis=1), tri, preferred_element_type=f32
                    )
                    wgt = jnp.exp2(jnp.minimum(z, 0.0) - soft + later + carry)
                    if j == i:
                        wgt = jnp.where(earlier, wgt, 0.0)
                    acc += jnp.dot(wgt.astype(bf16), vh[j, :, lanes], preferred_element_type=f32)
                    if j > 0:
                        carry += later[:, 0:1] + keep[:, 0:1]
                sums.append(acc)
            o = jnp.where(first, sums[0], sums[1])
            sq = o * o
            ms0 = jnp.sum(jnp.where(first, sq, 0.0), axis=1, keepdims=True)
            ms1 = jnp.sum(jnp.where(first, 0.0, sq), axis=1, keepdims=True)
            inv = jnp.where(
                first,
                lax.rsqrt(ms0 / head_size + eps_norm),
                lax.rsqrt(ms1 / head_size + eps_norm),
            )
            nout[i, :, lanes] = (o * inv).astype(bf16)

    pairs = cols // (2 * head_size)

    def attend_row(i, between):
        @pl.when(s != i)
        def _():
            for c in a_copies(s, i):
                c.wait_recv()

        for p in range(pairs):
            attend(i, p)
            for act_on in between[p : p + 1]:
                for stage, n in act_on:
                    stage(n)

        @pl.when(s != i)
        def _():
            r_copy(i, s).start()

        @pl.when(s == i)
        def _():
            ret[i] = nout[i]

    stage1(0)
    h_copy(0).start()
    h_copy(1).start()
    own_up_down(0)
    stage1(1)
    own_up_down(1)
    for t in (peers[1], peers[0], peers[2]):
        for c in a_copies(t, s):
            c.start()
    for c in local:
        c.wait()
    for stage, n in (
        (stage2, 0), (stage1, 2), (stage2, 1), (stage1, 3), (stage3, 0), (stage3, 1),
        (gate_block, 0), (stage2, 2), (stage2, 3), (stage3, 2), (gate_block, 1), (stage3, 3),
        (stage1, 4),
    ):
        stage(n)
    attend_row(0, ((), ((stage1, 5),)))
    attend_row(1, ((), ((stage2, 4), (stage2, 5))))
    attend_row(2, (((stage1, 6),), ((stage3, 4), (stage1, 7))))
    attend_row(3, (((stage3, 5), (gate_block, 2), (stage2, 6)), ((stage2, 7),)))
    gate_block(3)
    for t in peers:
        r_copy(s, t).wait_recv()
    out_block(0)
    out_block(1)
    out_block(2)
    stage3(7)
    out_block(3)

    for t in peers:
        for c in a_copies(t, s):
            c.wait_send()
        r_copy(t, s).wait_send()
    for n in range(2 * n_sp):
        for kind in (1,) if n % 2 == 0 else range(4):
            x_copy(kind, n).wait_send()
        for kind in (0, 2) if n % 2 == 0 else range(4):
            c_copy(kind, n).wait_send()
    for r in range(n_sp):
        p_copy(r).wait_send()
    for yy in range(2):
        h_copy(yy).wait_send()
    for w in range(2):

        @pl.when(s < n_sp - 1)
        def _():
            z_copy(w, s, 0, s + 1).wait_send()

        @pl.when(s > 0)
        def _():
            z_copy(w, s, 1, s - 1).wait_send()

        @pl.when(middle)
        def _():
            for r in range(1, n_sp):
                z_copy(w, order[r], 2 + r, forward_to(r)).wait_send()


def plane_shards(n_sp, n_dp, head_size, queries, key_rows, value_rows, break_offset, hidden_in, gate_weight, out_weight):
    rows, width = queries.shape[1:]
    heads_dev = break_offset.shape[2] // n_sp
    cols = width // n_sp
    depth = gate_weight.shape[0]
    offs = break_offset[0].T.reshape(n_sp, heads_dev, rows)
    vmem = pl.BlockSpec(memory_space=pltpu.VMEM)
    dma = pltpu.SemaphoreType.DMA
    mixed = pl.pallas_call(
        functools.partial(plane_kernel, n_sp, n_dp, head_size),
        out_shape=pltpu.VMEM((rows, hidden_in.shape[2]), bf16),
        in_specs=[pl.BlockSpec(memory_space=pl.ANY)] * 7,
        out_specs=vmem,
        scratch_shapes=[
            pltpu.VMEM((rows, depth * n_dp), bf16),
            pltpu.VMEM((2, n_dp, n_sp, 2, depth // 2, cols), bf16),
            pltpu.VMEM((n_sp, rows, cols), bf16),
            pltpu.VMEM((n_sp, rows, cols), bf16),
            pltpu.VMEM((n_sp, rows, cols), bf16),
            pltpu.VMEM((n_sp, heads_dev, rows), bf16),
            pltpu.VMEM((n_sp, rows, cols), bf16),
            pltpu.VMEM((n_sp, rows, cols), bf16),
            pltpu.VMEM((n_sp, rows, cols), f32),
            pltpu.VMEM((n_dp, rows, cols), f32),
            dma((4, n_sp)),
            dma((4, n_sp)),
            dma((n_sp,)),
            dma((n_sp,)),
            dma((2, 2 + n_sp)),
            dma((2, n_sp)),
            dma((4, 2 * n_sp)),
            dma((4, 2 * n_sp)),
            dma((4, 2 * n_sp)),
            dma((4, 2 * n_sp)),
            dma((9,)),
            pltpu.VMEM((2, rows, 2 * depth), bf16),
            pltpu.VMEM((n_sp, rows, cols), bf16),
            pltpu.VMEM((n_sp, rows, cols), bf16),
            dma((2,)),
            dma((2,)),
            dma((n_sp,)),
            dma((n_sp,)),
        ],
        compiler_params=pltpu.CompilerParams(
            collective_id=0, has_side_effects=True, vmem_limit_bytes=60 * 1024 * 1024
        ),
    )(queries[0], key_rows[0], value_rows[0], offs, hidden_in[0], gate_weight, out_weight)
    return mixed[None]


def planned(mesh, shards_general):
    n_sp, n_dp = mesh.shape["sp"], mesh.shape["dp"]

    def run(*local):
        queries, break_offset, gate_weight, out_weight = local[0], local[3], local[5], local[6]
        head_size = queries.shape[2] // break_offset.shape[2]
        cols = queries.shape[2] // n_sp
        if (
            n_sp == 4
            and n_dp == 8
            and queries.shape[0] == 1
            and queries.shape[1] == 128
            and 2 * head_size == 128
            and cols % 128 == 0
            and gate_weight.shape == out_weight.shape == (cols, cols)
        ):
            return plane_shards(n_sp, n_dp, head_size, *local)
        return shards_general(*local)

    return run


def solution(mesh):
    return jax.shard_map(
        planned(mesh, shards),
        mesh=mesh,
        in_specs=(
            P("dp", "sp", None),
            P("dp", "sp", None),
            P("dp", "sp", None),
            P("dp", "sp", None),
            P("dp", "sp", None),
            P("dp", "sp"),
            P("sp", "dp"),
        ),
        out_specs=P("dp", "sp", None),
        check_vma=False,
    )
```
